32 devices in a mesh: fs: 8 (over z, y), tp: 4 (over x, core).
Axes of the slice: x: 2, y: 2, z: 4, core: 2. Of those that a mesh axis runs over, the one named last changes fastest.
Arguments:
- inputs: bfloat16 [4608, 2048], P('fs'), may hold values from -6 to 6
- query_cotangent: bfloat16 [4608, 1024], P('fs', 'tp'), may hold values from -0.017944336 to 0.017944336
- value_cotangent: bfloat16 [4608, 1024], P('fs', 'tp'), may hold values from -0.017944336 to 0.017944336
- weights_query: float32 [2048, 1024], P('fs', 'tp'), may hold values from -6 to 6
- weights_value: float32 [2048, 1024], P('fs', 'tp'), may hold values from -6 to 6
- basis_query: bfloat16 [1024, 32], P('tp'), may hold values from -0.75 to 0.75
- basis_value: bfloat16 [1024, 32], P('tp'), may hold values from -0.75 to 0.75
- first_query: float32 [2048, 512], P('fs', 'tp'), may hold values from -5.4 to 5.4, as said below
- second_query: float32 [2048, 512], P('fs', 'tp'), may hold values from 0.05 to 1
- first_value: float32 [2048, 512], P('fs', 'tp'), may hold values from -5.4 to 5.4, as said below
- second_value: float32 [2048, 512], P('fs', 'tp'), may hold values from 0.05 to 1
Outputs:
- step_query: float32 [2048, 1024], P('fs', 'tp')
- step_value: float32 [2048, 1024], P('fs', 'tp')
- new_query: float32 [2048, 1024], P('fs', 'tp')
- new_value: float32 [2048, 1024], P('fs', 'tp')
- copy_query: bfloat16 [2048, 1024], P(None, 'tp')
- copy_value: bfloat16 [2048, 1024], P(None, 'tp')
- moment_query: float32 [2048, 512], P('fs', 'tp')
- square_query: float32 [2048, 512], P('fs', 'tp')
- moment_value: float32 [2048, 512], P('fs', 'tp')
- square_value: float32 [2048, 512], P('fs', 'tp')
The draws below stay inside these ranges and needn't reach their ends.
Inputs may be any that keep to these rules, and one draw needn't show every extreme that they name: `first_query`: first moments, with a spread of scale from row to row. `first_value`: first moments, with a spread of scale from row to row.
All inputs are finite; a program needn't handle non-finite values.
Results may differ from the reference program's by a relative error of at most 0.003.
Values may be sent and summed in bfloat16 or wider, within the bound.
A program may use at most 64 MiB of HBM per device.

```python
import math
import jax
import jax.numpy as jnp
from jax import lax

D = 2048
HEADS = 16
HEAD = 64
RK = 32
FW = 1024
TOKENS = 4608


def moment_draw(key):
    base = 0.3 * jnp.clip(jax.random.normal(jax.random.fold_in(key, 11), (D, HEADS * RK), jnp.float32), -4.0, 4.0)
    factor = jnp.exp(jax.random.uniform(jax.random.fold_in(key, 12), (D, 1), jnp.float32, -1.5, 1.5))
    return base * factor


def draw_first_query(key, part):
    return moment_draw(jax.random.fold_in(key, 1))


def draw_first_value(key, part):
    return moment_draw(jax.random.fold_in(key, 2))


def raised(drawn, own_key, source, target, parts, factor):
    owner, partner = [(jnp.arange(drawn.shape[position]) // (drawn.shape[position] // parts)).reshape([-1 if axis == position else 1 for axis in range(drawn.ndim)]) for position in (source, target)]
    chosen = jax.random.permutation(own_key, parts)[partner]
    strong = (owner == chosen) | (owner == (partner + parts // 2) % parts)
    return jnp.where(strong, factor * drawn, drawn)


def block_levels(rng, shape, cuts, smallest, high):
    level, own = 1.0, jax.random.fold_in(rng, 6)
    for axis_at, shards_of in cuts:
        heights = jnp.exp(jax.random.uniform(jax.random.fold_in(own, axis_at), (shards_of,), jnp.float32, smallest / len(cuts), high / len(cuts)))
        level = level * jnp.repeat(heights, shape[axis_at] // shards_of).reshape([-1 if axis == axis_at else 1 for axis in range(len(shape))])
    return level


def bell_draw(rng, dims, width, bound, cuts=(), held_as=jnp.bfloat16):
    entries = jax.random.normal(rng, dims, jnp.float32) * width
    if len(cuts) > 0:
        entries = block_levels(rng, dims, cuts, -0.22, 0.18) * entries
    return jnp.clip(entries, min=-bound, max=bound).astype(held_as)


def bell_draw_with(rng, extent, width, most, cuts, heavy, dtype=jnp.bfloat16):
    drawn = width * jax.random.normal(rng, extent, jnp.float32)
    if cuts:
        drawn = drawn * block_levels(rng, extent, cuts, -0.22, 0.18)
    return jnp.clip(raised(drawn, jax.random.fold_in(rng, 3), *heavy), -most, most).astype(dtype)


def setup_inputs(seed: int = 0) -> dict:
    key_list = jax.random.split(jax.random.key(seed), 12)
    inputs = bell_draw_with(key_list[0], (TOKENS, D), 1.0, 6.0, ((0, 8),), (0, 1, 8, 2.0))
    query_cotangent = bell_draw(key_list[1], (TOKENS, FW), 0.003, 0.017944336, ((0, 8), (1, 4)))
    value_cotangent = bell_draw(key_list[2], (TOKENS, FW), 0.003, 0.017944336, ((0, 8), (1, 4)))
    weights_query = bell_draw(key_list[3], (D, FW), 1.0, 6.0, ((0, 8), (1, 4)), jnp.float32)
    weights_value = bell_draw(key_list[4], (D, FW), 1.0, 6.0, ((0, 8), (1, 4)), jnp.float32)
    basis_query = bell_draw(key_list[5], (FW, RK), HEAD ** -0.5, 0.75, ((0, 4),))
    basis_value = bell_draw(key_list[6], (FW, RK), HEAD ** -0.5, 0.75, ((0, 4),))
    first_query = draw_first_query(jax.random.fold_in(key_list[11], 71), 0)
    second_query = jnp.clip(jnp.exp(math.log(1.0) - 2.9957323 * jax.random.uniform(key_list[8], (D, HEADS * RK), jnp.float32) ** block_levels(key_list[8], (D, HEADS * RK), ((0, 8), (1, 4)), -0.2, 0.2)), 0.05, 1.0)
    first_value = draw_first_value(jax.random.fold_in(key_list[11], 71), 0)
    second_value = jnp.clip(jnp.exp(math.log(1.0) - 2.9957323 * jax.random.uniform(key_list[10], (D, HEADS * RK), jnp.float32) ** block_levels(key_list[10], (D, HEADS * RK), ((0, 8), (1, 4)), -0.2, 0.2)), 0.05, 1.0)
    return {"inputs": inputs, "query_cotangent": query_cotangent, "value_cotangent": value_cotangent, "weights_query": weights_query, "weights_value": weights_value, "basis_query": basis_query, "basis_value": basis_value, "first_query": first_query, "second_query": second_query, "first_value": first_value, "second_value": second_value}


def apply_basis(gradient, basis):
    split = gradient.reshape(D, HEADS, HEAD)
    factor = basis.reshape(HEADS, HEAD, RK).astype(jnp.float32)
    out = jnp.einsum('nhd,hdr->nhr', split, factor, precision=lax.Precision.HIGHEST)
    return out.reshape(D, HEADS * RK)

def expand(direction, basis):
    split = direction.reshape(D, HEADS, RK)
    factor = basis.reshape(HEADS, HEAD, RK).astype(jnp.float32)
    out = jnp.einsum('nhr,hdr->nhd', split, factor, precision=lax.Precision.HIGHEST)
    return out.reshape(D, HEADS * HEAD)

def update(inputs, cotangent, weights, basis, first, second):
    gradient = jnp.dot(inputs.T, cotangent, preferred_element_type=jnp.float32)
    reduced = apply_basis(gradient, basis)
    moment = 0.9 * first + 0.1 * reduced
    square = 0.95 * second + 0.05 * reduced * reduced
    direction = moment / (jnp.sqrt(square) + 1e-08)
    scale = 1.0 / jnp.sqrt(jnp.mean(direction * direction) + 0.25)
    step = scale * expand(direction, basis)
    fresh = weights - 0.1 * step
    return (step, fresh, fresh.astype(jnp.bfloat16), moment, square)

def reference(inputs, query_cotangent, value_cotangent, weights_query, weights_value, basis_query, basis_value, first_query, second_query, first_value, second_value):
    step_q, new_q, copy_q, moment_q, square_q = update(inputs, query_cotangent, weights_query, basis_query, first_query, second_query)
    step_v, new_v, copy_v, moment_v, square_v = update(inputs, value_cotangent, weights_value, basis_value, first_value, second_value)
    return (step_q, step_v, new_q, new_v, copy_q, copy_v, moment_q, square_q, moment_v, square_v)
```

```python
import functools

import jax
import jax.numpy as jnp
from jax import lax
from jax.experimental import pallas as pl
from jax.experimental.pallas import tpu as pltpu
from jax.sharding import PartitionSpec as P

HEAD = 64
RK = 32
MESH = pl.DeviceIdType.MESH
F32 = jnp.float32
BF16 = jnp.bfloat16


def flip(x, bits):
    out, weight = x, 1
    while weight <= bits:
        if bits & weight:
            out = out + weight * (1 - 2 * ((x // weight) % 2))
        weight *= 2
    return out


def remote(src, dst, send, recv, to):
    return pltpu.make_async_remote_copy(
        src_ref=src, dst_ref=dst, send_sem=send, recv_sem=recv, device_id=to, device_id_type=MESH
    )


def body(
    n,
    t,
    x_hbm,
    cq_hbm,
    cv_hbm,
    wq_hbm,
    wv_hbm,
    bq_hbm,
    bv_hbm,
    fq_hbm,
    sq_hbm,
    fv_hbm,
    sv_hbm,
    stepq_hbm,
    stepv_hbm,
    newq_hbm,
    newv_hbm,
    copyq_hbm,
    copyv_hbm,
    momq_hbm,
    sqrq_hbm,
    momv_hbm,
    sqrv_hbm,
    x,
    cot,
    w,
    basis,
    first,
    second,
    small,
    part,
    summed,
    arrived1,
    arrived2,
    raw,
    step,
    new,
    mom,
    sqr,
    tot,
    tot_all,
    copy,
    in_sem,
    out_sem,
    s1,
    r1,
    s2,
    r2,
    st,
    rt,
    su,
    ru,
    sd,
    rd,
    sy,
    ry,
    so,
):
    f = lax.axis_index("fs")
    g = lax.axis_index("tp")
    me = f * t + g
    count = n * t
    outer = n // 2
    a, b = f // 2, f % 2
    mate = (a * 2 + 1 - b, g)
    depth = x.shape[1]
    rows = depth // n
    cols = w.shape[2]
    wide = cols // HEAD * RK

    barrier = pltpu.get_barrier_semaphore()

    def greet(i, c):
        j = (me + 1 + i) % count
        pl.semaphore_signal(barrier, inc=1, device_id=(j // t, j % t), device_id_type=MESH)
        return c

    lax.fori_loop(0, count - 1, greet, 0)

    loads = [
        pltpu.make_async_copy(src, dst, in_sem.at[i])
        for i, (src, dst) in enumerate(
            (
                (bq_hbm, basis.at[0]),
                (bv_hbm, basis.at[1]),
                (cq_hbm, cot.at[0]),
                (cv_hbm, cot.at[1]),
                (x_hbm, x),
                (fq_hbm, first.at[0]),
                (fv_hbm, first.at[1]),
                (sq_hbm, second.at[0]),
                (sv_hbm, second.at[1]),
                (wq_hbm, w.at[0]),
                (wv_hbm, w.at[1]),
            )
        )
    ]
    for load in loads:
        load.start()
    for load in loads[:4]:
        load.wait()

    spread = (
        lax.broadcasted_iota(jnp.int32, (RK, wide), 1) % RK
        == lax.broadcasted_iota(jnp.int32, (RK, wide), 0)
    ).astype(BF16)
    own_head = (
        lax.broadcasted_iota(jnp.int32, (cols, wide), 0) // HEAD
        == lax.broadcasted_iota(jnp.int32, (cols, wide), 1) // RK
    )
    diag = [
        jnp.where(own_head, jnp.dot(basis[p], spread, preferred_element_type=F32), 0.0).astype(BF16)
        for p in range(2)
    ]
    for p in range(2):
        small[:, p * wide : (p + 1) * wide] = jnp.dot(
            cot[p], diag[p], preferred_element_type=F32
        ).astype(BF16)
    loads[4].wait()

    chunk = max(2 * rows, min(depth, 256))
    chunks = depth // chunk
    pairs = chunk // (2 * rows)
    order = list(range(chunks // 2, chunks)) + list(range(chunks // 2 - 1, -1, -1))
    at = a // pairs

    def part_rows(z, half):
        return pl.ds(pl.multiple_of((z * 2 + half) * rows, rows), rows)

    def first_copy(k, i):
        z = flip(at, order[k]) * pairs + i
        return remote(
            part.at[part_rows(z, 1 - b)],
            arrived1.at[z],
            s1.at[k * pairs + i],
            r1.at[k * pairs + i],
            mate,
        )

    for k in range(chunks):
        c = flip(at, order[k])
        part[pl.ds(pl.multiple_of(c * chunk, chunk), chunk), :] = lax.dot_general(
            x[:, pl.ds(pl.multiple_of(c * chunk, chunk), chunk)],
            small[...],
            (((0,), (0,)), ((), ())),
            preferred_element_type=F32,
        ).astype(BF16)
        if k == 0:
            pl.semaphore_wait(barrier, count - 1)
        for i in range(pairs):
            first_copy(k, i).start()

    def second_copy(k, i):
        z = flip(at, order[k]) * pairs + i
        return z, remote(
            summed.at[z], arrived2.at[a], s2.at[k * pairs + i], r2.at[a], (z * 2 + b, g)
        )

    for k in range(chunks):
        for i in range(pairs):
            first_copy(k, i).wait_recv()
            z, onward = second_copy(k, i)
            if k < chunks - 1 or pairs > 1:
                summed[z] = (
                    part[part_rows(z, b), :].astype(F32) + arrived1[z].astype(F32)
                ).astype(BF16)
                if k < chunks - 1:
                    onward.start()
                else:
                    pl.when(z != a)(onward.start)

    total = part[part_rows(a, b), :].astype(F32) + arrived1[a].astype(F32)
    for p in range(outer - 1, 0, -1):
        src = flip(a, p)
        remote(summed.at[src], arrived2.at[src], s2.at[0], r2.at[src], (src * 2 + b, g)).wait_recv()
        total = total + arrived2[src].astype(F32)

    for load in loads[5:]:
        load.wait()
    for p in range(2):
        reduced = total[:, p * wide : (p + 1) * wide]
        moment = 0.9 * first[p] + 0.1 * reduced
        square = 0.95 * second[p] + 0.05 * reduced * reduced
        direction = moment / (jnp.sqrt(square) + 1e-08)
        mom[p] = moment
        sqr[p] = square
        tot[0, :, p * wide : (p + 1) * wide] = jnp.sum(direction * direction, axis=0, keepdims=True)
        first[p] = direction
    tot_all[me] = tot[0]

    def total_copy(i):
        j = (me + 1 + i) % count
        return remote(tot.at[0], tot_all.at[me], st.at[i], rt.at[me], (j // t, j % t))

    def send_total(i, c):
        total_copy(i).start()
        return c

    lax.fori_loop(0, count - 1, send_total, 0)

    stores = [
        pltpu.make_async_copy(src, dst, out_sem.at[i])
        for i, (src, dst) in enumerate(
            (
                (mom.at[0], momq_hbm),
                (mom.at[1], momv_hbm),
                (sqr.at[0], sqrq_hbm),
                (sqr.at[1], sqrv_hbm),
                (step.at[0], stepq_hbm),
                (step.at[1], stepv_hbm),
                (new.at[0], newq_hbm),
                (new.at[1], newv_hbm),
            )
        )
    ]
    for s in stores[:4]:
        s.start()

    back = (((1,), (1,)), ((), ()))
    for p in range(2):
        direction = first[p]
        upper = direction.astype(BF16)
        lower = (direction - upper.astype(F32)).astype(BF16)
        raw[p] = lax.dot_general(upper, diag[p], back, preferred_element_type=F32) + lax.dot_general(
            lower, diag[p], back, preferred_element_type=F32
        )

    def await_total(i, c):
        j = (me + 1 + i) % count
        remote(tot.at[0], tot_all.at[j], st.at[i], rt.at[j], (j // t, j % t)).wait_recv()
        return c

    lax.fori_loop(0, count - 1, await_total, 0)
    sums = jnp.sum(tot_all[...], axis=0)
    entries = depth * wide * t

    def block(z, half):
        return pl.ds(pl.multiple_of((z * 2 + half) * rows, rows), rows)

    up_to, down_to = (f + 2, g), (f - 2, g)

    def up(k, p):
        rows_at = block(a - k, b)
        ref = copy.at[p, rows_at]
        return remote(ref, ref, su.at[k, p], ru.at[k, p], up_to)

    def down(k, p):
        ref = copy.at[p, block(a + k, b)]
        return remote(ref, ref, sd.at[k, p], rd.at[k, p], down_to)

    def up_in(k, p):
        ref = copy.at[p, block(a - 1 - k, b)]
        return remote(ref, ref, su.at[k, p], ru.at[k, p], up_to)

    def down_in(k, p):
        ref = copy.at[p, block(a + 1 + k, b)]
        return remote(ref, ref, sd.at[k, p], rd.at[k, p], down_to)

    def across(z, p):
        ref = copy.at[p, block(z, b)]
        return remote(ref, ref, sy.at[z, p], ry.at[z, p], mate)

    def across_in(z, p):
        ref = copy.at[p, block(z, 1 - b)]
        return remote(ref, ref, sy.at[z, p], ry.at[z, p], mate)

    def out(z, half, p):
        at_rows = block(z, half)
        return pltpu.make_async_copy(
            copy.at[p, at_rows], (copyq_hbm, copyv_hbm)[p].at[at_rows], so.at[z, half, p]
        )

    for p in range(2):
        mean = jnp.sum(sums[:, p * wide : (p + 1) * wide], axis=1, keepdims=True) / entries
        scale = 1.0 / jnp.sqrt(mean + 0.25)
        step[p] = scale * raw[p]
        new[p] = w[p] - 0.1 * step[p]
        copy[p, block(a, b)] = new[p].astype(BF16)
        pl.when(a < outer - 1)(up(0, p).start)
        pl.when(a > 0)(down(0, p).start)
        across(a, p).start()
    for s in stores[4:]:
        s.start()
    for p in range(2):
        out(a, b, p).start()

    for k in range(outer - 1):
        for p in range(2):

            @pl.when(a - 1 - k >= 0)
            def _():
                up_in(k, p).wait_recv()
                if k + 1 < outer - 1:
                    pl.when(a < outer - 1)(up(k + 1, p).start)
                across(a - 1 - k, p).start()
                out(a - 1 - k, b, p).start()

            @pl.when(a + 1 + k <= outer - 1)
            def _():
                down_in(k, p).wait_recv()
                if k + 1 < outer - 1:
                    pl.when(a > 0)(down(k + 1, p).start)
                across(a + 1 + k, p).start()
                out(a + 1 + k, b, p).start()

    for k in range(outer):
        for p in range(2):

            if k == 0:
                across_in(a, p).wait_recv()
                out(a, 1 - b, p).start()
            else:

                @pl.when(a - k >= 0)
                def _():
                    across_in(a - k, p).wait_recv()
                    out(a - k, 1 - b, p).start()

                @pl.when(a + k <= outer - 1)
                def _():
                    across_in(a + k, p).wait_recv()
                    out(a + k, 1 - b, p).start()

    for k in range(chunks):
        for i in range(pairs):
            first_copy(k, i).wait_send()
            z, onward = second_copy(k, i)
            if k < chunks - 1:
                onward.wait_send()
            elif pairs > 1:
                pl.when(z != a)(onward.wait_send)

    def sent_total(i, c):
        total_copy(i).wait_send()
        return c

    lax.fori_loop(0, count - 1, sent_total, 0)
    for k in range(outer - 1):
        for p in range(2):
            pl.when(jnp.logical_and(a - k >= 0, a < outer - 1))(up(k, p).wait_send)
            pl.when(jnp.logical_and(a + k <= outer - 1, a > 0))(down(k, p).wait_send)
    for z in range(outer):
        for p in range(2):
            across(z, p).wait_send()
            for half in range(2):
                out(z, half, p).wait()
    for s in stores:
        s.wait()


def per_device(n, t, *args):
    x, cq, _, wq, _, bq, _, fq = args[:8]
    tokens, depth = x.shape
    rows, cols = wq.shape
    wide = fq.shape[1]
    outer = n // 2
    chunk = max(2 * rows, min(depth, 256))
    hbm = pl.BlockSpec(memory_space=pl.ANY)
    shape = jax.ShapeDtypeStruct
    dma = pltpu.SemaphoreType.DMA
    full, half = shape((rows, cols), F32), shape((rows, wide), F32)
    whole = shape((depth, cols), BF16)
    return pl.pallas_call(
        functools.partial(body, n, t),
        out_shape=(full, full, full, full, whole, whole, half, half, half, half),
        in_specs=[hbm] * 11,
        out_specs=[hbm] * 10,
        scratch_shapes=[
            pltpu.VMEM((tokens, depth), BF16),
            pltpu.VMEM((2, tokens, cols), BF16),
            pltpu.VMEM((2, rows, cols), F32),
            pltpu.VMEM((2, cols, RK), BF16),
            pltpu.VMEM((2, rows, wide), F32),
            pltpu.VMEM((2, rows, wide), F32),
            pltpu.VMEM((tokens, 2 * wide), BF16),
            pltpu.VMEM((depth, 2 * wide), BF16),
            pltpu.VMEM((outer, rows, 2 * wide), BF16),
            pltpu.VMEM((outer, rows, 2 * wide), BF16),
            pltpu.VMEM((outer, rows, 2 * wide), BF16),
            pltpu.VMEM((2, rows, cols), F32),
            pltpu.VMEM((2, rows, cols), F32),
            pltpu.VMEM((2, rows, cols), F32),
            pltpu.VMEM((2, rows, wide), F32),
            pltpu.VMEM((2, rows, wide), F32),
            pltpu.VMEM((1, 1, 2 * wide), F32),
            pltpu.VMEM((n * t, 1, 2 * wide), F32),
            pltpu.VMEM((2, depth, cols), BF16),
            dma((11,)),
            dma((8,)),
            dma((outer,)),
            dma((outer,)),
            dma((outer,)),
            dma((outer,)),
            dma((n * t,)),
            dma((n * t,)),
            dma((outer, 2)),
            dma((outer, 2)),
            dma((outer, 2)),
            dma((outer, 2)),
            dma((outer, 2)),
            dma((outer, 2)),
            dma((outer, 2, 2)),
        ],
        compiler_params=pltpu.CompilerParams(collective_id=0, has_side_effects=True),
        name="update",
    )(*args)


def solution(mesh):
    split = P("fs", "tp")
    return jax.shard_map(
        functools.partial(per_device, mesh.shape["fs"], mesh.shape["tp"]),
        mesh=mesh,
        in_specs=(P("fs", None),) + (split,) * 4 + (P("tp", None),) * 2 + (split,) * 4,
        out_specs=(split,) * 4 + (P(None, "tp"),) * 2 + (split,) * 4,
        check_vma=False,
    )
```

```python
import functools

import jax
import jax.numpy as jnp
from jax import lax
from jax.experimental import pallas as pl
from jax.experimental.pallas import tpu as pltpu
from jax.sharding import PartitionSpec as P

HEAD = 64
RK = 32
MESH = pl.DeviceIdType.MESH
F32 = jnp.float32
BF16 = jnp.bfloat16


def flip(x, bits):
    out, weight = x, 1
    while weight <= bits:
        if bits & weight:
            out = out + weight * (1 - 2 * ((x // weight) % 2))
        weight *= 2
    return out


def remote(src, dst, send, recv, to):
    return pltpu.make_async_remote_copy(
        src_ref=src, dst_ref=dst, send_sem=send, recv_sem=recv, device_id=to, device_id_type=MESH
    )


def body(
    n,
    t,
    x_hbm,
    cq_hbm,
    cv_hbm,
    wq_hbm,
    wv_hbm,
    bq_hbm,
    bv_hbm,
    fq_hbm,
    sq_hbm,
    fv_hbm,
    sv_hbm,
    step,
    new,
    copy,
    mom,
    sqr,
    x,
    cot,
    w,
    basis,
    first,
    second,
    small,
    part,
    summed,
    arrived1,
    arrived2,
    raw,
    tot,
    tot_all,
    in_sem,
    s1,
    r1,
    s2,
    r2,
    st,
    rt,
    su,
    ru,
    sd,
    rd,
    sy,
    ry,
):
    f = lax.axis_index("fs")
    g = lax.axis_index("tp")
    me = f * t + g
    count = n * t
    outer = n // 2
    a, b = f // 2, f % 2
    mate = (a * 2 + 1 - b, g)
    depth = x.shape[1]
    rows = depth // n
    cols = w.shape[2]
    wide = cols // HEAD * RK

    barrier = pltpu.get_barrier_semaphore()

    def greet(i, c):
        j = (me + 1 + i) % count
        pl.semaphore_signal(barrier, inc=1, device_id=(j // t, j % t), device_id_type=MESH)
        return c

    lax.fori_loop(0, count - 1, greet, 0)

    loads = [
        pltpu.make_async_copy(src, dst, in_sem.at[i])
        for i, (src, dst) in enumerate(
            (
                (bq_hbm, basis.at[0]),
                (bv_hbm, basis.at[1]),
                (cq_hbm, cot.at[0]),
                (cv_hbm, cot.at[1]),
                (x_hbm, x),
                (fq_hbm, first.at[0]),
                (fv_hbm, first.at[1]),
                (sq_hbm, second.at[0]),
                (sv_hbm, second.at[1]),
                (wq_hbm, w.at[0]),
                (wv_hbm, w.at[1]),
            )
        )
    ]
    for load in loads:
        load.start()
    for load in loads[:4]:
        load.wait()

    spread = (
        lax.broadcasted_iota(jnp.int32, (RK, wide), 1) % RK
        == lax.broadcasted_iota(jnp.int32, (RK, wide), 0)
    ).astype(BF16)
    own_head = (
        lax.broadcasted_iota(jnp.int32, (cols, wide), 0) // HEAD
        == lax.broadcasted_iota(jnp.int32, (cols, wide), 1) // RK
    )
    diag = [
        jnp.where(
            own_head,
            lax.dot_general(basis[p], spread, (((0,), (0,)), ((), ())), preferred_element_type=F32),
            0.0,
        ).astype(BF16)
        for p in range(2)
    ]
    for p in range(2):
        small[:, p * wide : (p + 1) * wide] = jnp.dot(
            cot[p], diag[p], preferred_element_type=F32
        ).astype(BF16)
    loads[4].wait()

    chunk = max(2 * rows, min(depth, 256))
    chunks = depth // chunk
    pairs = chunk // (2 * rows)
    order = list(range(chunks // 2, chunks)) + list(range(chunks // 2 - 1, -1, -1))
    at = a // pairs

    def part_rows(z, half):
        return pl.ds(pl.multiple_of((z * 2 + half) * rows, rows), rows)

    def first_copy(k, i):
        z = flip(at, order[k]) * pairs + i
        return remote(
            part.at[part_rows(z, 1 - b)],
            arrived1.at[z],
            s1.at[k * pairs + i],
            r1.at[k * pairs + i],
            mate,
        )

    for k in range(chunks):
        c = flip(at, order[k])
        part[pl.ds(pl.multiple_of(c * chunk, chunk), chunk), :] = lax.dot_general(
            x[:, pl.ds(pl.multiple_of(c * chunk, chunk), chunk)],
            small[...],
            (((0,), (0,)), ((), ())),
            preferred_element_type=F32,
        ).astype(BF16)
        if k == 0:
            pl.semaphore_wait(barrier, count - 1)
        for i in range(pairs):
            first_copy(k, i).start()

    def second_copy(k, i):
        z = flip(at, order[k]) * pairs + i
        return z, remote(
            summed.at[z], arrived2.at[a], s2.at[k * pairs + i], r2.at[a], (z * 2 + b, g)
        )

    for k in range(chunks):
        for i in range(pairs):
            first_copy(k, i).wait_recv()
            z, onward = second_copy(k, i)
            if k < chunks - 1 or pairs > 1:
                summed[z] = (
                    part[part_rows(z, b), :].astype(F32) + arrived1[z].astype(F32)
                ).astype(BF16)
                if k < chunks - 1:
                    onward.start()
                else:
                    pl.when(z != a)(onward.start)

    total = part[part_rows(a, b), :].astype(F32) + arrived1[a].astype(F32)
    for p in range(outer - 1, 0, -1):
        src = flip(a, p)
        remote(summed.at[src], arrived2.at[src], s2.at[0], r2.at[src], (src * 2 + b, g)).wait_recv()
        total = total + arrived2[src].astype(F32)

    for load in loads[5:]:
        load.wait()
    for p in range(2):
        reduced = total[:, p * wide : (p + 1) * wide]
        moment = 0.9 * first[p] + 0.1 * reduced
        square = 0.95 * second[p] + 0.05 * reduced * reduced
        direction = moment / (jnp.sqrt(square) + 1e-08)
        mom[p] = moment
        sqr[p] = square
        tot[0, :, p * wide : (p + 1) * wide] = jnp.sum(direction * direction, axis=0, keepdims=True)
        first[p] = direction
    tot_all[me] = tot[0]

    def total_copy(i):
        j = (me + 1 + i) % count
        return remote(tot.at[0], tot_all.at[me], st.at[i], rt.at[me], (j // t, j % t))

    def send_total(i, c):
        total_copy(i).start()
        return c

    lax.fori_loop(0, count - 1, send_total, 0)

    back = (((1,), (1,)), ((), ()))
    for p in range(2):
        direction = first[p]
        upper = direction.astype(BF16)
        lower = (direction - upper.astype(F32)).astype(BF16)
        raw[p] = lax.dot_general(upper, diag[p], back, preferred_element_type=F32) + lax.dot_general(
            lower, diag[p], back, preferred_element_type=F32
        )

    def await_total(i, c):
        j = (me + 1 + i) % count
        remote(tot.at[0], tot_all.at[j], st.at[i], rt.at[j], (j // t, j % t)).wait_recv()
        return c

    lax.fori_loop(0, count - 1, await_total, 0)
    sums = jnp.sum(tot_all[...], axis=0)
    entries = depth * wide * t

    def block(z, half):
        return pl.ds(pl.multiple_of((z * 2 + half) * rows, rows), rows)

    up_to, down_to = (f + 2, g), (f - 2, g)

    def up(k, p):
        rows_at = block(a - k, b)
        ref = copy.at[p, rows_at]
        return remote(ref, ref, su.at[k, p], ru.at[k, p], up_to)

    def down(k, p):
        ref = copy.at[p, block(a + k, b)]
        return remote(ref, ref, sd.at[k, p], rd.at[k, p], down_to)

    def up_in(k, p):
        ref = copy.at[p, block(a - 1 - k, b)]
        return remote(ref, ref, su.at[k, p], ru.at[k, p], up_to)

    def down_in(k, p):
        ref = copy.at[p, block(a + 1 + k, b)]
        return remote(ref, ref, sd.at[k, p], rd.at[k, p], down_to)

    def across(z, p):
        ref = copy.at[p, block(z, b)]
        return remote(ref, ref, sy.at[z, p], ry.at[z, p], mate)

    def across_in(z, p):
        ref = copy.at[p, block(z, 1 - b)]
        return remote(ref, ref, sy.at[z, p], ry.at[z, p], mate)

    for p in range(2):
        mean = jnp.sum(sums[:, p * wide : (p + 1) * wide], axis=1, keepdims=True) / entries
        scale = 1.0 / jnp.sqrt(mean + 0.25)
        step[p] = scale * raw[p]
        new[p] = w[p] - 0.1 * step[p]
        copy[p, block(a, b)] = new[p].astype(BF16)
        pl.when(a < outer - 1)(up(0, p).start)
        pl.when(a > 0)(down(0, p).start)
        across(a, p).start()

    for k in range(outer - 1):
        for p in range(2):

            @pl.when(a - 1 - k >= 0)
            def _():
                up_in(k, p).wait_recv()
                if k + 1 < outer - 1:
                    pl.when(a < outer - 1)(up(k + 1, p).start)
                across(a - 1 - k, p).start()

            @pl.when(a + 1 + k <= outer - 1)
            def _():
                down_in(k, p).wait_recv()
                if k + 1 < outer - 1:
                    pl.when(a > 0)(down(k + 1, p).start)
                across(a + 1 + k, p).start()

    for k in range(outer):
        for p in range(2):

            if k == 0:
                across_in(a, p).wait_recv()
            else:

                @pl.when(a - k >= 0)
                def _():
                    across_in(a - k, p).wait_recv()

                @pl.when(a + k <= outer - 1)
                def _():
                    across_in(a + k, p).wait_recv()

    for k in range(chunks):
        for i in range(pairs):
            first_copy(k, i).wait_send()
            z, onward = second_copy(k, i)
            if k < chunks - 1:
                onward.wait_send()
            elif pairs > 1:
                pl.when(z != a)(onward.wait_send)

    def sent_total(i, c):
        total_copy(i).wait_send()
        return c

    lax.fori_loop(0, count - 1, sent_total, 0)
    for k in range(outer - 1):
        for p in range(2):
            pl.when(jnp.logical_and(a - k >= 0, a < outer - 1))(up(k, p).wait_send)
            pl.when(jnp.logical_and(a + k <= outer - 1, a > 0))(down(k, p).wait_send)
    for z in range(outer):
        for p in range(2):
            across(z, p).wait_send()


def store(step, new, copy, mom, sqr, *rest):
    outs, sem = rest[:10], rest[10]
    srcs = [ref.at[p] for ref in (step, new, copy, mom, sqr) for p in range(2)]
    order = (4, 5, 0, 1, 2, 3, 6, 7, 8, 9)
    moves = [pltpu.make_async_copy(srcs[i], outs[i], sem.at[i]) for i in order]
    for move in moves:
        move.start()
    for move in moves:
        move.wait()


def per_device(n, t, x, cq, cv, wq, wv, bq, bv, fq, sq, fv, sv):
    tokens, depth = x.shape
    rows, cols = wq.shape
    wide = fq.shape[1]
    outer = n // 2
    hbm = pl.BlockSpec(memory_space=pltpu.HBM)
    vmem = pl.BlockSpec(memory_space=pltpu.VMEM)
    shape = jax.ShapeDtypeStruct
    dma = pltpu.SemaphoreType.DMA
    kept = (
        pltpu.VMEM((2, rows, cols), F32),
        pltpu.VMEM((2, rows, cols), F32),
        pltpu.VMEM((2, depth, cols), BF16),
        pltpu.VMEM((2, rows, wide), F32),
        pltpu.VMEM((2, rows, wide), F32),
    )
    held = pl.pallas_call(
        functools.partial(body, n, t),
        out_shape=kept,
        in_specs=[hbm] * 11,
        out_specs=[vmem] * 5,
        scratch_shapes=[
            pltpu.VMEM((tokens, depth), BF16),
            pltpu.VMEM((2, tokens, cols), BF16),
            pltpu.VMEM((2, rows, cols), F32),
            pltpu.VMEM((2, RK, cols), BF16),
            pltpu.VMEM((2, rows, wide), F32),
            pltpu.VMEM((2, rows, wide), F32),
            pltpu.VMEM((tokens, 2 * wide), BF16),
            pltpu.VMEM((depth, 2 * wide), BF16),
            pltpu.VMEM((outer, rows, 2 * wide), BF16),
            pltpu.VMEM((outer, rows, 2 * wide), BF16),
            pltpu.VMEM((outer, rows, 2 * wide), BF16),
            pltpu.VMEM((2, rows, cols), F32),
            pltpu.VMEM((1, 1, 2 * wide), F32),
            pltpu.VMEM((n * t, 1, 2 * wide), F32),
            dma((11,)),
            dma((outer,)),
            dma((outer,)),
            dma((outer,)),
            dma((outer,)),
            dma((n * t,)),
            dma((n * t,)),
            dma((outer, 2)),
            dma((outer, 2)),
            dma((outer, 2)),
            dma((outer, 2)),
            dma((outer, 2)),
            dma((outer, 2)),
        ],
        compiler_params=pltpu.CompilerParams(
            collective_id=0, has_side_effects=True, vmem_limit_bytes=40 * 2**20
        ),
        name="update",
    )(x, cq, cv, wq, wv, bq.T, bv.T, fq, sq, fv, sv)
    full, half = shape((rows, cols), F32), shape((rows, wide), F32)
    whole = shape((depth, cols), BF16)
    outs = pl.pallas_call(
        store,
        out_shape=(full,) * 4 + (whole,) * 2 + (half,) * 4,
        in_specs=[vmem] * 5,
        out_specs=[hbm] * 10,
        scratch_shapes=[dma((10,))],
        compiler_params=pltpu.CompilerParams(vmem_limit_bytes=40 * 2**20),
        name="store",
    )(*held)
    return tuple(outs[i] for i in (0, 1, 2, 3, 4, 5, 6, 8, 7, 9))


def solution(mesh):
    split = P("fs", "tp")
    return jax.shard_map(
        functools.partial(per_device, mesh.shape["fs"], mesh.shape["tp"]),
        mesh=mesh,
        in_specs=(P("fs", None),) + (split,) * 4 + (P("tp", None),) * 2 + (split,) * 4,
        out_specs=(split,) * 4 + (P(None, "tp"),) * 2 + (split,) * 4,
        check_vma=False,
    )
```

```python
import functools

import jax
import jax.numpy as jnp
from jax import lax
from jax.experimental import pallas as pl
from jax.experimental.pallas import tpu as pltpu
from jax.sharding import PartitionSpec as P

HEAD = 64
RK = 32
MESH = pl.DeviceIdType.MESH
F32 = jnp.float32
BF16 = jnp.bfloat16


def flip(x, bits):
    out, weight = x, 1
    while weight <= bits:
        if bits & weight:
            out = out + weight * (1 - 2 * ((x // weight) % 2))
        weight *= 2
    return out


def remote(src, dst, send, recv, to):
    return pltpu.make_async_remote_copy(
        src_ref=src, dst_ref=dst, send_sem=send, recv_sem=recv, device_id=to, device_id_type=MESH
    )


def body(
    n,
    t,
    x_hbm,
    cq_hbm,
    cv_hbm,
    wq_hbm,
    wv_hbm,
    bq_hbm,
    bv_hbm,
    fq_hbm,
    sq_hbm,
    fv_hbm,
    sv_hbm,
    step,
    new,
    copy,
    mom,
    sqr,
    x,
    cot,
    w,
    basis,
    first,
    second,
    small,
    part,
    summed,
    arrived1,
    arrived2,
    raw,
    tot,
    tot_all,
    in_sem,
    s1,
    r1,
    s2,
    r2,
    st,
    rt,
    su,
    ru,
    sd,
    rd,
    sy,
    ry,
    sn,
    rn,
):
    f = lax.axis_index("fs")
    g = lax.axis_index("tp")
    me = f * t + g
    count = n * t
    outer = n // 2
    a, b = f // 2, f % 2
    mate = (a * 2 + 1 - b, g)
    depth = x.shape[1]
    rows = depth // n
    cols = w.shape[2]
    wide = cols // HEAD * RK

    barrier = pltpu.get_barrier_semaphore()

    def greet(i, c):
        j = (me + 1 + i) % count
        pl.semaphore_signal(barrier, inc=1, device_id=(j // t, j % t), device_id_type=MESH)
        return c

    lax.fori_loop(0, count - 1, greet, 0)

    loads = [
        pltpu.make_async_copy(src, dst, in_sem.at[i])
        for i, (src, dst) in enumerate(
            (
                (bq_hbm, basis.at[0]),
                (bv_hbm, basis.at[1]),
                (cq_hbm, cot.at[0]),
                (cv_hbm, cot.at[1]),
                (x_hbm, x),
                (fq_hbm, first.at[0]),
                (fv_hbm, first.at[1]),
                (sq_hbm, second.at[0]),
                (sv_hbm, second.at[1]),
                (wq_hbm, w.at[0]),
                (wv_hbm, w.at[1]),
            )
        )
    ]
    for load in loads:
        load.start()
    for load in loads[:4]:
        load.wait()

    spread = (
        lax.broadcasted_iota(jnp.int32, (RK, wide), 1) % RK
        == lax.broadcasted_iota(jnp.int32, (RK, wide), 0)
    ).astype(BF16)
    own_head = (
        lax.broadcasted_iota(jnp.int32, (cols, wide), 0) // HEAD
        == lax.broadcasted_iota(jnp.int32, (cols, wide), 1) // RK
    )
    diag = [
        jnp.where(
            own_head,
            lax.dot_general(basis[p], spread, (((0,), (0,)), ((), ())), preferred_element_type=F32),
            0.0,
        ).astype(BF16)
        for p in range(2)
    ]
    for p in range(2):
        small[:, p * wide : (p + 1) * wide] = jnp.dot(
            cot[p], diag[p], preferred_element_type=F32
        ).astype(BF16)
    loads[4].wait()

    chunk = max(2 * rows, min(depth, 256))
    chunks = depth // chunk
    pairs = chunk // (2 * rows)
    order = list(range(chunks // 2, chunks)) + list(range(chunks // 2 - 1, -1, -1))
    at = a // pairs

    def part_rows(z, half):
        return pl.ds(pl.multiple_of((z * 2 + half) * rows, rows), rows)

    def first_copy(k, i, p):
        z = flip(at, order[k]) * pairs + i
        return remote(
            part.at[p, part_rows(z, 1 - b)],
            arrived1.at[p, z],
            s1.at[k * pairs + i, p],
            r1.at[k * pairs + i, p],
            mate,
        )

    for k in range(chunks):
        here = pl.ds(pl.multiple_of(flip(at, order[k]) * chunk, chunk), chunk)
        sums = lax.dot_general(
            x[:, here], small[...], (((0,), (0,)), ((), ())), preferred_element_type=F32
        ).astype(BF16)
        for p in range(2):
            part[p, here] = sums[:, p * wide : (p + 1) * wide]
        if k == 0:
            pl.semaphore_wait(barrier, count - 1)
        for i in range(pairs):
            first_copy(k, i, 0).start()
    for k in range(chunks):
        for i in range(pairs):
            first_copy(k, i, 1).start()

    def second_copy(k, i, p):
        z = flip(at, order[k]) * pairs + i
        return z, remote(
            summed.at[p, z],
            arrived2.at[p, a],
            s2.at[k * pairs + i, p],
            r2.at[a, p],
            (z * 2 + b, g),
        )

    def total_copy(i, p):
        j = (me + 1 + i) % count
        return remote(
            tot.at[p, 0], tot_all.at[p, me], st.at[p, i], rt.at[p, me], (j // t, j % t)
        )

    back = (((1,), (1,)), ((), ()))

    def reduce(p):
        for k in range(chunks):
            for i in range(pairs):
                first_copy(k, i, p).wait_recv()
                if k < chunks - 1 or pairs > 1:
                    z, onward = second_copy(k, i, p)
                    summed[p, z] = (
                        part[p, part_rows(z, b)].astype(F32) + arrived1[p, z].astype(F32)
                    ).astype(BF16)
                    if k < chunks - 1:
                        onward.start()
                    else:
                        pl.when(z != a)(onward.start)
        reduced = part[p, part_rows(a, b)].astype(F32) + arrived1[p, a].astype(F32)
        for q in range(outer - 1, 0, -1):
            src = flip(a, q)
            remote(
                summed.at[p, src],
                arrived2.at[p, src],
                s2.at[0, p],
                r2.at[src, p],
                (src * 2 + b, g),
            ).wait_recv()
            reduced = reduced + arrived2[p, src].astype(F32)
        if p == 0:
            for load in loads[5:]:
                load.wait()
        moment = 0.9 * first[p] + 0.1 * reduced
        square = 0.95 * second[p] + 0.05 * reduced * reduced
        direction = moment / (jnp.sqrt(square) + 1e-08)
        tot[p, 0] = jnp.sum(direction * direction, axis=0, keepdims=True)

        def send_total(i, c):
            total_copy(i, p).start()
            return c

        lax.fori_loop(0, count - 1, send_total, 0)
        tot_all[p, me] = tot[p, 0]
        mom[p] = moment
        sqr[p] = square
        upper = direction.astype(BF16)
        lower = (direction - upper.astype(F32)).astype(BF16)
        raw[p] = lax.dot_general(upper, diag[p], back, preferred_element_type=F32) + lax.dot_general(
            lower, diag[p], back, preferred_element_type=F32
        )

    entries = depth * wide * t

    def block(z, half):
        return pl.ds(pl.multiple_of((z * 2 + half) * rows, rows), rows)

    up_to, down_to = (f + 2, g), (f - 2, g)

    def up(k, p):
        rows_at = block(a - k, b)
        ref = copy.at[p, rows_at]
        return remote(ref, ref, su.at[k, p], ru.at[k, p], up_to)

    def down(k, p):
        ref = copy.at[p, block(a + k, b)]
        return remote(ref, ref, sd.at[k, p], rd.at[k, p], down_to)

    def up_in(k, p):
        ref = copy.at[p, block(a - 1 - k, b)]
        return remote(ref, ref, su.at[k, p], ru.at[k, p], up_to)

    def down_in(k, p):
        ref = copy.at[p, block(a + 1 + k, b)]
        return remote(ref, ref, sd.at[k, p], rd.at[k, p], down_to)

    def across(z, p):
        ref = copy.at[p, block(z, b)]
        return remote(ref, ref, sy.at[z, p], ry.at[z, p], mate)

    def across_in(z, p):
        ref = copy.at[p, block(z, 1 - b)]
        return remote(ref, ref, sy.at[z, p], ry.at[z, p], mate)

    near = flip(a, 1)

    def beside(z):
        ref = copy.at[1, block(z, 1 - b)]
        return remote(ref, ref, sn.at[0], rn.at[0], (near * 2 + b, g))

    def finish(p):
        def await_total(i, c):
            j = (me + 1 + i) % count
            remote(
                tot.at[p, 0], tot_all.at[p, j], st.at[p, i], rt.at[p, j], (j // t, j % t)
            ).wait_recv()
            return c

        lax.fori_loop(0, count - 1, await_total, 0)
        mean = jnp.sum(jnp.sum(tot_all[p], axis=0), axis=1, keepdims=True) / entries
        scale = 1.0 / jnp.sqrt(mean + 0.25)
        move = scale * raw[p]
        fresh = w[p] - 0.1 * move
        copy[p, block(a, b)] = fresh.astype(BF16)
        pl.when(a < outer - 1)(lambda: up(0, p).start())
        pl.when(a > 0)(lambda: down(0, p).start())
        across(a, p).start()
        step[p] = move
        new[p] = fresh

    def forward(k, p):
        @pl.when(a - 1 - k >= 0)
        def _():
            up_in(k, p).wait_recv()
            if k + 1 < outer - 1:
                pl.when(a < outer - 1)(lambda: up(k + 1, p).start())
            if k == 0 and p == 1:
                pl.when(a % 2 == 0)(lambda: across(a - 1, p).start())
            else:
                across(a - 1 - k, p).start()

        @pl.when(a + 1 + k <= outer - 1)
        def _():
            down_in(k, p).wait_recv()
            if k + 1 < outer - 1:
                pl.when(a > 0)(lambda: down(k + 1, p).start())
            if k == 0 and p == 1:
                pl.when(a % 2 == 1)(lambda: across(a + 1, p).start())
            else:
                across(a + 1 + k, p).start()

    reduce(0)
    reduce(1)
    finish(0)
    forward(0, 0)
    finish(1)
    for k in range(outer - 1):
        if k + 1 < outer - 1:
            forward(k + 1, 0)
        forward(k, 1)
        if k == 0:
            across_in(a, 1).wait_recv()
            beside(a).start()

    for z in range(outer):
        for p in range(2):
            if p == 0:
                across_in(z, p).wait_recv()
                across(z, p).wait_send()
            else:
                pl.when(jnp.logical_and(z != near, z != a))(lambda: across_in(z, 1).wait_recv())
                pl.when(z != near)(lambda: across(z, 1).wait_send())
    beside(near).wait_recv()
    beside(a).wait_send()

    for p in range(2):
        for k in range(chunks):
            for i in range(pairs):
                first_copy(k, i, p).wait_send()
                if k < chunks - 1:
                    second_copy(k, i, p)[1].wait_send()
                elif pairs > 1:
                    z, onward = second_copy(k, i, p)
                    pl.when(z != a)(onward.wait_send)

        def sent_total(i, c):
            total_copy(i, p).wait_send()
            return c

        lax.fori_loop(0, count - 1, sent_total, 0)
        for k in range(outer - 1):
            pl.when(jnp.logical_and(a - k >= 0, a < outer - 1))(lambda: up(k, p).wait_send())
            pl.when(jnp.logical_and(a + k <= outer - 1, a > 0))(lambda: down(k, p).wait_send())


def store(step, new, copy, mom, sqr, *rest):
    outs, sem = rest[:10], rest[10]
    srcs = [ref.at[p] for ref in (step, new, copy, mom, sqr) for p in range(2)]
    order = (4, 5, 0, 1, 2, 3, 6, 7, 8, 9)
    moves = [pltpu.make_async_copy(srcs[i], outs[i], sem.at[i]) for i in order]
    for move in moves:
        move.start()
    for move in moves:
        move.wait()


def per_device(n, t, x, cq, cv, wq, wv, bq, bv, fq, sq, fv, sv):
    tokens, depth = x.shape
    rows, cols = wq.shape
    wide = fq.shape[1]
    outer = n // 2
    hbm = pl.BlockSpec(memory_space=pltpu.HBM)
    vmem = pl.BlockSpec(memory_space=pltpu.VMEM)
    shape = jax.ShapeDtypeStruct
    dma = pltpu.SemaphoreType.DMA
    kept = (
        pltpu.VMEM((2, rows, cols), F32),
        pltpu.VMEM((2, rows, cols), F32),
        pltpu.VMEM((2, depth, cols), BF16),
        pltpu.VMEM((2, rows, wide), F32),
        pltpu.VMEM((2, rows, wide), F32),
    )
    held = pl.pallas_call(
        functools.partial(body, n, t),
        out_shape=kept,
        in_specs=[hbm] * 11,
        out_specs=[vmem] * 5,
        scratch_shapes=[
            pltpu.VMEM((tokens, depth), BF16),
            pltpu.VMEM((2, tokens, cols), BF16),
            pltpu.VMEM((2, rows, cols), F32),
            pltpu.VMEM((2, RK, cols), BF16),
            pltpu.VMEM((2, rows, wide), F32),
            pltpu.VMEM((2, rows, wide), F32),
            pltpu.VMEM((tokens, 2 * wide), BF16),
            pltpu.VMEM((2, depth, wide), BF16),
            pltpu.VMEM((2, outer, rows, wide), BF16),
            pltpu.VMEM((2, outer, rows, wide), BF16),
            pltpu.VMEM((2, outer, rows, wide), BF16),
            pltpu.VMEM((2, rows, cols), F32),
            pltpu.VMEM((2, 1, 1, wide), F32),
            pltpu.VMEM((2, n * t, 1, wide), F32),
            dma((11,)),
            dma((outer, 2)),
            dma((outer, 2)),
            dma((outer, 2)),
            dma((outer, 2)),
            dma((2, n * t)),
            dma((2, n * t)),
            dma((outer, 2)),
            dma((outer, 2)),
            dma((outer, 2)),
            dma((outer, 2)),
            dma((outer, 2)),
            dma((outer, 2)),
            dma((1,)),
            dma((1,)),
        ],
        compiler_params=pltpu.CompilerParams(
            collective_id=0, has_side_effects=True, vmem_limit_bytes=62 * 10**6
        ),
        name="update",
    )(x, cq, cv, wq, wv, bq.T, bv.T, fq, sq, fv, sv)
    full, half = shape((rows, cols), F32), shape((rows, wide), F32)
    whole = shape((depth, cols), BF16)
    outs = pl.pallas_call(
        store,
        out_shape=(full,) * 4 + (whole,) * 2 + (half,) * 4,
        in_specs=[vmem] * 5,
        out_specs=[hbm] * 10,
        scratch_shapes=[dma((10,))],
        compiler_params=pltpu.CompilerParams(vmem_limit_bytes=40 * 2**20),
        name="store",
    )(*held)
    return tuple(outs[i] for i in (0, 1, 2, 3, 4, 5, 6, 8, 7, 9))


def solution(mesh):
    split = P("fs", "tp")
    return jax.shard_map(
        functools.partial(per_device, mesh.shape["fs"], mesh.shape["tp"]),
        mesh=mesh,
        in_specs=(P("fs", None),) + (split,) * 4 + (P("tp", None),) * 2 + (split,) * 4,
        out_specs=(split,) * 4 + (P(None, "tp"),) * 2 + (split,) * 4,
        check_vma=False,
    )
```
